256 devices in a mesh: sp: 64 (over z, x, core), tp: 4 (over y).
Axes of the slice: x: 4, y: 4, z: 8, core: 2. Of those that a mesh axis runs over, the one named last changes fastest.
Arguments:
- glu_a: bfloat16 [16384, 1024], P('sp', 'tp'), may hold values from -6 to 6
- glu_b: bfloat16 [16384, 1024], P('sp', 'tp'), may hold values from -6 to 6
- saved_conv: bfloat16 [16384, 1024], P('sp', 'tp')
- taps: float32 [31, 1024], P(None, 'tp'), may hold values from -1 to 1
- norm_gain_vector: float32 [1024], P('tp'), may hold values from 0.1 to 1.9
- out_proj: bfloat16 [1024, 2048], P('tp'), may hold values from -0.1875 to 0.1875
- moe_in: bfloat16 [16384, 2048], P('sp'), may hold values from -6 to 6
- grad_out: bfloat16 [16384, 2048], P('sp'), may hold values from -16 to 16
- expert_ids: int32 [16384, 2], P('sp'), may hold values from 0 to 63, all different within a row; in each aligned block of 256 rows (0 to 255, 256 to 511, ...) at most 12 rows name the same one
- route_weights: float32 [16384, 2], P('sp'), may hold values from 0.3 to 2
- w_gate: bfloat16 [64, 2048, 1024], P('sp', None, 'tp'), may hold values from -0.125 to 0.125
- w_up: bfloat16 [64, 2048, 1024], P('sp', None, 'tp'), may hold values from -0.125 to 0.125
- w_down: bfloat16 [64, 1024, 2048], P('sp', 'tp'), may hold values from -0.1875 to 0.1875
Outputs:
- grad_glu_a: bfloat16 [16384, 1024], P('sp', 'tp')
- grad_glu_b: bfloat16 [16384, 1024], P('sp', 'tp')
- grad_out_proj: float32 [2048, 1024], P('sp', 'tp')
- grad_gate: bfloat16 [64, 2048, 1024], P('sp', None, 'tp')
- grad_up: bfloat16 [64, 2048, 1024], P('sp', None, 'tp')
- grad_down: bfloat16 [64, 1024, 2048], P('sp', 'tp')
The draws below stay inside these ranges and needn't reach their ends.
Inputs may be any that keep to these rules, and one draw needn't show every extreme that they name: `expert_ids`: in each aligned block of 256 tokens, a token's 2 experts differ, and no expert is named more than 12 times; some expert reaches 12 in some blocks.
All inputs are finite; a program needn't handle non-finite values.
Results may differ from the reference program's by a relative error of at most 0.015.
Values may be sent and summed in bfloat16 or wider, within the bound.
No kernel may reach another device: no remote copies, remote signals or barrier semaphores. Data moves between devices by JAX's collectives and lax.ppermute only.
A program may use at most 64 MiB of HBM per device.

```python
import math
import jax
import jax.numpy as jnp
import numpy as np
from jax import lax

D = 2048
CONV_CHANNELS = 1024
FF = 1024
KW = 31
TOPK = 2
TOK_DEV = 256
TOKENS = 16384
EXPERTS = 64
CAP = 12
N_SP = 64
N_TP = 4


def draw_saved_conv(key, part):
    key_base = jax.random.fold_in(key, 11)
    key_row = jax.random.fold_in(key, 12)
    key_chan = jax.random.fold_in(key, 13)
    base = jax.random.normal(key_base, (TOKENS, CONV_CHANNELS), jnp.float32)
    rising = jnp.exp(jnp.log(4.0) * jnp.arange(CONV_CHANNELS, dtype=jnp.float32) / CONV_CHANNELS)
    rough = jax.random.uniform(key_chan, (CONV_CHANNELS,), jnp.float32, 0.5, 1.5)
    row_scale = jax.random.uniform(key_row, (TOKENS, 1), jnp.float32, 0.6, 1.6)
    values = base * rising[None, :] * rough[None, :] * row_scale * 0.5
    return values.astype(jnp.bfloat16)


def raised(array, key, source, target, shards_of, factor):
    owner, partner = [(jnp.arange(array.shape[axis_at]) // (array.shape[axis_at] // shards_of)).reshape([-1 if axis == axis_at else 1 for axis in range(array.ndim)]) for axis_at in (source, target)]
    chosen = jax.random.permutation(key, shards_of)[partner]
    strong = (owner == chosen) | (owner == (partner + shards_of // 2) % shards_of)
    return jnp.where(strong, factor * array, array)


def block_scale(stream_key, shape, split, least, top_value):
    def one(dim, parts):
        heights = jax.random.uniform(jax.random.fold_in(jax.random.fold_in(stream_key, 6), dim), (parts,), jnp.float32, least / len(split), top_value / len(split))
        return jnp.repeat(jnp.exp(heights), shape[dim] // parts).reshape((-1,) + (1,) * (len(shape) - dim - 1))

    loudness = one(*split[0])
    for cut in split[1:]:
        loudness = loudness * one(*cut)
    return loudness


def deal_out(key, own, number, rows, number_of, top, limit, lean):
    order = jax.random.permutation(key, number_of)
    packed, usual = shares(number_of, rows * top, limit, lean, True), shares(number_of, rows * top, limit, lean, False)
    places = jnp.arange(number_of)

    def named(lengths, rotation):
        used = int((lengths > 0).sum())
        fixed = max(1, used // 4)
        moved = fixed + (places - fixed + rotation * (used - fixed)) % max(1, number_of - fixed)
        return jnp.zeros((number_of,), jnp.int32).at[order[jnp.where(places < fixed, places, moved)]].set(jnp.asarray(lengths, jnp.int32))

    lengths = jnp.where(number % 4 == 0, named(packed, number // 4), named(usual, number - number // 4 - 1))
    mixed = jax.random.permutation(jax.random.fold_in(own, 3), number_of)
    source_of, receiver = mixed[0:number_of // 2 * 2:2], mixed[1:number_of // 2 * 2:2]
    room = jnp.minimum(lengths[source_of] - 1, limit - lengths[receiver]) // 2
    room = jnp.where((source_of == order[0]) | (receiver == order[0]) | (lengths[receiver] == 0), 0, jnp.maximum(room, 0))
    moved = jax.random.randint(jax.random.fold_in(own, 4), (number_of // 2,), 0, 1 << 20) % (room + 1)
    lengths = lengths.at[source_of].add(-moved).at[receiver].add(moved)
    items = jnp.searchsorted(jnp.cumsum(lengths), jnp.arange(rows * top), side="right").astype(jnp.int32)
    table = items.reshape(top, rows).T
    table = table[jax.random.permutation(jax.random.fold_in(own, 1), rows)]
    rotation = jax.random.randint(jax.random.fold_in(own, 2), (rows, 1), 0, top)
    return jnp.take_along_axis(table, (jnp.arange(top)[None, :] + rotation) % top, axis=1)


def shares(count, total, limit, lean, full):
    weights = [(1 << 20) // math.isqrt(grade ** lean) + 1 for grade in range(1, count + 1)]
    largest = limit if full else min(limit, max(-(-total // count), total * weights[0] // sum(weights)))
    least = 1 if total - largest >= count - 1 else 0
    given, surplus = [largest] + [least] * (count - 1), total - largest - least * (count - 1)
    while surplus > 0:
        free = [i for i in range(1, count) if given[i] < largest] or [i for i in range(1, count) if given[i] < limit]
        whole, remaining = sum([weights[i] for i in free]), surplus
        for i in free:
            more = min(limit - given[i], max(1, remaining * weights[i] // whole), surplus)
            given[i] = given[i] + more
            surplus = surplus - more
    return np.array(given)


def normal_values(rng, shape, deviation, most, shards=(), held_as=jnp.bfloat16):
    factor_of = block_scale(rng, shape, shards, -0.22, 0.18) if shards else 1.0
    drawn = jax.random.normal(rng, shape, jnp.float32) * deviation * factor_of
    return jnp.minimum(jnp.maximum(drawn, -most), most).astype(held_as)


def gaussian_with(rng, dims, deviation, limit, shards, heavy, kind=jnp.bfloat16):
    result = deviation * jax.random.normal(rng, dims, jnp.float32)
    if shards:
        result = result * block_scale(rng, dims, shards, -0.22, 0.18)
    return jnp.clip(raised(result, jax.random.fold_in(rng, 3), *heavy), -limit, limit).astype(kind)


def setup_inputs(seed: int = 0) -> dict:
    streams_of = jax.random.split(jax.random.key(seed), 14)
    glu_a = normal_values(streams_of[0], (TOKENS, CONV_CHANNELS), 1.0, 6.0, ((0, 64), (1, 4)))
    glu_b = normal_values(streams_of[1], (TOKENS, CONV_CHANNELS), 1.0, 6.0, ((0, 64), (1, 4)))
    saved_conv = draw_saved_conv(jax.random.fold_in(streams_of[13], 71), 0)
    taps = normal_values(streams_of[3], (KW, CONV_CHANNELS), 0.18, 1.0, ((1, 4),), jnp.float32)
    norm_gain_vector = jnp.clip(1.0 + 0.18 * jax.random.normal(streams_of[4], (CONV_CHANNELS,), jnp.float32), 0.1, 1.9)
    out_proj = normal_values(streams_of[5], (CONV_CHANNELS, D), CONV_CHANNELS ** -0.5, 0.1875, ((0, 4),))
    moe_in = normal_values(streams_of[6], (TOKENS, D), 1.0, 6.0, ((0, 64),))
    grad_out = gaussian_with(streams_of[7], (TOKENS, D), 1.0, 16.0, ((0, 64),), (0, 1, 64, 4.0))
    expert_ids_keys = jax.random.split(jax.random.fold_in(streams_of[8], 1), TOKENS // TOK_DEV)
    expert_ids_turns = jax.random.permutation(jax.random.fold_in(streams_of[8], 3), TOKENS // TOK_DEV)
    expert_ids = jax.vmap(lambda own, number: deal_out(jax.random.fold_in(streams_of[8], 2), own, number, TOK_DEV, EXPERTS, TOPK, CAP, 1))(expert_ids_keys, expert_ids_turns).reshape((TOKENS, TOPK))
    route_weights = jnp.clip(0.3 + 1.7 * jax.random.uniform(streams_of[9], (TOKENS, TOPK), jnp.float32) ** block_scale(streams_of[9], (TOKENS, TOPK), ((0, 64),), -0.2, 0.2), 0.3, 2.0)
    w_gate = normal_values(streams_of[10], (EXPERTS, D, FF), D ** -0.5, 0.125, ((0, 64), (2, 4)))
    w_up = normal_values(streams_of[11], (EXPERTS, D, FF), D ** -0.5, 0.125, ((0, 64), (2, 4)))
    w_down = normal_values(streams_of[12], (EXPERTS, FF, D), FF ** -0.5, 0.1875, ((0, 64), (1, 4)))
    return {"glu_a": glu_a, "glu_b": glu_b, "saved_conv": saved_conv, "taps": taps, "norm_gain_vector": norm_gain_vector, "out_proj": out_proj, "moe_in": moe_in, "grad_out": grad_out, "expert_ids": expert_ids, "route_weights": route_weights, "w_gate": w_gate, "w_up": w_up, "w_down": w_down}


def expert_backward(item):
    in_rows, cot_rows, gate_w, up_w, down_w = item
    gate_pre = jnp.dot(in_rows, gate_w, preferred_element_type=jnp.float32)
    up_pre = jnp.dot(in_rows, up_w, preferred_element_type=jnp.float32)
    sig_gate = jax.nn.sigmoid(gate_pre)
    act_gate = gate_pre * sig_gate
    hidden = (act_gate * up_pre).astype(jnp.bfloat16)
    grad_hidden = jnp.dot(cot_rows, down_w.T, preferred_element_type=jnp.float32)
    grad_upact = (grad_hidden * act_gate).astype(jnp.bfloat16)
    grad_gateact = (grad_hidden * up_pre * sig_gate * (1.0 + gate_pre * (1.0 - sig_gate))).astype(jnp.bfloat16)
    grad_down = jnp.dot(hidden.T, cot_rows, preferred_element_type=jnp.float32).astype(jnp.bfloat16)
    grad_gate = jnp.dot(in_rows.T, grad_gateact, preferred_element_type=jnp.float32).astype(jnp.bfloat16)
    grad_up = jnp.dot(in_rows.T, grad_upact, preferred_element_type=jnp.float32).astype(jnp.bfloat16)
    rows_n = in_rows.shape[0]
    part_ff = FF // N_TP
    g_split = grad_gateact.astype(jnp.float32).reshape(rows_n, N_TP, part_ff)
    u_split = grad_upact.astype(jnp.float32).reshape(rows_n, N_TP, part_ff)
    wg_split = gate_w.astype(jnp.float32).reshape(D, N_TP, part_ff)
    wu_split = up_w.astype(jnp.float32).reshape(D, N_TP, part_ff)
    partial_value = jnp.einsum('sqf,dqf->qsd', g_split, wg_split) + jnp.einsum('sqf,dqf->qsd', u_split, wu_split)
    partial_value = partial_value.astype(jnp.bfloat16).astype(jnp.float32)
    row_grads = lax.optimization_barrier(jnp.sum(partial_value, axis=0)).astype(jnp.bfloat16)
    return (grad_gate, grad_up, grad_down, row_grads)

def reference(glu_a, glu_b, saved_conv, taps, norm_gain_vector, out_proj, moe_in, grad_out, expert_ids, route_weights, w_gate, w_up, w_down):
    per_expert = N_SP * CAP
    pairs = TOKENS * TOPK
    flat_ids = expert_ids.reshape(N_SP, TOK_DEV * TOPK)
    onehot = (flat_ids[:, :, None] == jnp.arange(EXPERTS, dtype=jnp.int32)[None, None, :]).astype(jnp.int32)
    slot_rank = lax.optimization_barrier(jnp.sum((jnp.cumsum(onehot, axis=1) - onehot) * onehot, axis=2))
    source = jnp.arange(N_SP, dtype=jnp.int32)[:, None]
    slots = (flat_ids * per_expert + source * CAP + slot_rank).reshape(pairs).astype(jnp.int32)
    owner_idx = jnp.full((EXPERTS * per_expert,), pairs, jnp.int32).at[slots].set(jnp.arange(pairs, dtype=jnp.int32))
    token_idx = owner_idx // TOPK
    in_pad = jnp.concatenate([moe_in, jnp.zeros((1, D), jnp.bfloat16)], axis=0)
    in_rows = in_pad[token_idx].reshape(EXPERTS, per_expert, D)
    scaled = (grad_out.astype(jnp.float32)[:, None, :] * route_weights[:, :, None]).astype(jnp.bfloat16)
    cot_pad = jnp.concatenate([scaled.reshape(pairs, D), jnp.zeros((1, D), jnp.bfloat16)], axis=0)
    cot_rows = cot_pad[owner_idx].reshape(EXPERTS, per_expert, D)
    grad_gate, grad_up, grad_down, row_grads = lax.map(expert_backward, (in_rows, cot_rows, w_gate, w_up, w_down))
    picked = row_grads.reshape(EXPERTS * per_expert, D)[slots].reshape(TOKENS, TOPK, D)
    grad_moe = lax.optimization_barrier(jnp.sum(picked.astype(jnp.float32), axis=1))
    grad_mix = (grad_out.astype(jnp.float32) + grad_moe).astype(jnp.bfloat16)
    head_gradient = jnp.dot(grad_mix, out_proj.T, preferred_element_type=jnp.float32)
    convolved_rows = saved_conv.astype(jnp.float32)
    channel_average = lax.optimization_barrier(jnp.mean(convolved_rows, axis=1, keepdims=True))
    var_c = lax.optimization_barrier(jnp.mean(convolved_rows * convolved_rows, axis=1, keepdims=True)) - channel_average * channel_average
    inverse_deviation = lax.rsqrt(var_c + 1e-05)
    centered_scaled = (convolved_rows - channel_average) * inverse_deviation
    normalized_rows = centered_scaled * norm_gain_vector[None, :]
    sigmoid_of_norm = jax.nn.sigmoid(normalized_rows)
    heads = (normalized_rows * sigmoid_of_norm).astype(jnp.bfloat16)
    grad_out_proj = jnp.dot(grad_mix.T, heads, preferred_element_type=jnp.float32)
    normalized_gradient = head_gradient * sigmoid_of_norm * (1.0 + normalized_rows * (1.0 - sigmoid_of_norm)) * norm_gain_vector[None, :]
    gradient_average = lax.optimization_barrier(jnp.mean(normalized_gradient, axis=1, keepdims=True))
    product_average = lax.optimization_barrier(jnp.mean(normalized_gradient * centered_scaled, axis=1, keepdims=True))
    convolved_gradient = (inverse_deviation * (normalized_gradient - gradient_average - centered_scaled * product_average)).astype(jnp.bfloat16)
    reach = (KW - 1) // 2
    padded = jnp.pad(convolved_gradient, ((reach, reach), (0, 0))).astype(jnp.float32)
    grad_y = jnp.zeros((TOKENS, CONV_CHANNELS), jnp.float32)
    for tap_idx in range(KW):
        grad_y = grad_y + taps[tap_idx][None, :] * padded[2 * reach - tap_idx:2 * reach - tap_idx + TOKENS]
    sig_b = jax.nn.sigmoid(glu_b.astype(jnp.float32))
    grad_glu_a = (grad_y * sig_b).astype(jnp.bfloat16)
    grad_glu_b = (grad_y * glu_a.astype(jnp.float32) * sig_b * (1.0 - sig_b)).astype(jnp.bfloat16)
    return (grad_glu_a, grad_glu_b, grad_out_proj, grad_gate, grad_up, grad_down)
```

```python
import jax
import jax.numpy as jnp
from jax import lax
from jax.experimental import pallas as pl
from jax.experimental.pallas import tpu as pltpu
from jax.sharding import PartitionSpec as P


CONV_CHANNELS = 1024
F32 = jnp.float32
BF16 = jnp.bfloat16
CAP = 12
HALF = 256
ROWS = 8
WIDE = 768


NN = (((1,), (0,)), ((), ()))
NT = (((1,), (1,)), ((), ()))
TN = (((0,), (0,)), ((), ()))


def dot(a, b, dims=NN):
    return lax.dot_general(a, b, dims, preferred_element_type=F32)


def shift(x, k, axis="tp"):
    n = lax.axis_size(axis)
    return lax.ppermute(x, axis, [(i, (i + k) % n) for i in range(n)])


def slot_ids(row):
    e = jnp.floor((row + 0.5) * (1.0 / ROWS))
    r = row - ROWS * e
    second = r >= 4
    return e * CAP + r, e * CAP + 8 + jnp.where(second, r - 4, r), second


def dispatch_kernel(q_ref, ids_ref, w_ref, moe_ref, go_ref, in_ref, cot_ref, slot_ref):
    n_exp = in_ref.shape[0] // ROWS
    tok = ids_ref.shape[1]
    e_iota = lax.broadcasted_iota(jnp.int32, (n_exp, tok), 0)
    ids0, ids1 = ids_ref[0:1, :], ids_ref[1:2, :]
    oh0 = jnp.where(e_iota == ids0, 1.0, 0.0)
    oh1 = jnp.where(e_iota == ids1, 1.0, 0.0)
    earlier = jnp.where(
        lax.broadcasted_iota(jnp.int32, (tok, tok), 0) < lax.broadcasted_iota(jnp.int32, (tok, tok), 1),
        1.0,
        0.0,
    ).astype(BF16)
    count = dot((oh0 + oh1).astype(BF16), earlier)
    slot0 = ids0.astype(F32) * CAP + jnp.sum(count * oh0, axis=0, keepdims=True)
    slot1 = ids1.astype(F32) * CAP + jnp.sum(count * oh1, axis=0, keepdims=True)
    slot_ref[0:1, :] = slot0
    slot_ref[1:2, :] = slot1
    w0, w1 = w_ref[0:1, :], w_ref[1:2, :]
    step = 256

    @pl.loop(0, in_ref.shape[0] // step)
    def _(i):
        at = pl.multiple_of(i * step, step)
        rows = pl.ds(at, step)
        row = (lax.broadcasted_iota(jnp.int32, (step, tok), 0) + at).astype(F32)
        slot_a, slot_b, second = slot_ids(row)

        def fill(slot, lanes, pick):
            hit0, hit1 = slot == slot0, slot == slot1
            select = jnp.where(hit0 | hit1, 1.0, 0.0).astype(BF16)
            weight = jnp.sum(jnp.where(hit0, w0, 0.0) + jnp.where(hit1, w1, 0.0), axis=1, keepdims=True)
            in_ref[rows, lanes] = pick(dot(select, moe_ref[...])).astype(BF16)
            cot_ref[rows, lanes] = (pick(dot(select, go_ref[...])) * weight).astype(BF16)

        fill(slot_a, pl.ds(0, 2 * HALF), lambda v: v)
        fill(slot_b, pl.ds(2 * HALF, HALF), lambda v: jnp.where(second, v[:, HALF:], v[:, :HALF]))


def dispatch(q, ids_t, w_t, moe_in, grad_out, n_exp):
    tok, _ = moe_in.shape
    rows = n_exp * ROWS
    small = pl.BlockSpec((2, tok), lambda i, q: (0, 0))
    quarter = pl.BlockSpec((tok, 2 * HALF), lambda i, q: (0, q[0]))
    out = pl.BlockSpec((rows, WIDE), lambda i, q: (0, 0))
    return pl.pallas_call(
        dispatch_kernel,
        grid_spec=pltpu.PrefetchScalarGridSpec(
            num_scalar_prefetch=1,
            grid=(1,),
            in_specs=[small, small, quarter, quarter],
            out_specs=[out, out, small],
        ),
        out_shape=[
            jax.ShapeDtypeStruct((rows, WIDE), BF16),
            jax.ShapeDtypeStruct((rows, WIDE), BF16),
            jax.ShapeDtypeStruct((2, tok), F32),
        ],
        name="dispatch",
    )(q, ids_t, w_t, moe_in, grad_out)


def whole(n):
    return [pl.BlockSpec(memory_space=pltpu.VMEM)] * n


def at_quarter(q_ref, j, h=0, size=HALF):
    return pl.ds(pl.multiple_of(lax.rem(q_ref[0] + j, 4) * (2 * HALF) + h * HALF, HALF), size)


def lanes(k, n=1):
    return pl.ds(k * HALF, n * HALF)


def total(parts):
    out = None
    for p in parts:
        out = p if out is None else out + p
    return out


def roll_rows(x, k):
    return pltpu.roll(x, k % x.shape[0], axis=0)


def lined_up(first, second):
    row = lax.broadcasted_iota(jnp.int32, first.shape, 0)
    return jnp.where((row & 7) < 4, first + roll_rows(second, -4), 0.0)


def contract(xs, w, dims):
    both = total(dot(x[:, lanes(0, 2)], w(j, 0, 2), dims) for j, x in enumerate(xs))
    first = total(dot(x[:, lanes(2)], w(j, 0, 1), dims) for j, x in enumerate(xs))
    second = total(dot(x[:, lanes(2)], w(j, 1, 1), dims) for j, x in enumerate(xs))
    return both, lined_up(first, second)


def pre_kernel(q_ref, *refs):
    xs, (wg_ref, wu_ref), (gate_ref, up_ref) = refs[:8], refs[8:10], refs[10:]
    for g in range(2):
        rows = pl.ds(g * HALF, HALF)
        for w_ref, o_ref in ((wg_ref, gate_ref), (wu_ref, up_ref)):
            a, b = contract(xs[g::2], lambda j, h, n: w_ref[at_quarter(q_ref, j, h, n * HALF), :], NN)
            o_ref[rows, lanes(0)] = a
            o_ref[rows, lanes(1)] = b


def row_parts(q_ref, gg, gu, wg_ref, wu_ref, j, o_ref):
    both, h0, h1 = at_quarter(q_ref, j, 0, 2 * HALF), at_quarter(q_ref, j, 0), at_quarter(q_ref, j, 1)
    o_ref[:, lanes(0, 2)] = (
        dot(gg[:, :HALF], wg_ref[both, :], NT) + dot(gu[:, :HALF], wu_ref[both, :], NT)
    ).astype(BF16)
    gg_b, gu_b = gg[:, HALF:], gu[:, HALF:]
    o_ref[:, lanes(2)] = (
        (dot(gg_b, wg_ref[h0, :], NT) + dot(gu_b, wu_ref[h0, :], NT))
        + (dot(moved(gg_b), wg_ref[h1, :], NT) + dot(moved(gu_b), wu_ref[h1, :], NT))
    ).astype(BF16)


def moved(x):
    return roll_rows(x.astype(F32), 4).astype(BF16)


def act_kernel(q_ref, *refs):
    cs, (wd_ref, wg_ref, wu_ref, gate_ref, up_ref) = refs[:8], refs[8:13]
    hid_ref, gu_ref, gg_ref = refs[13:16]
    outs = refs[16:]
    for g in range(2):
        rows = pl.ds(g * HALF, HALF)
        gh = jnp.concatenate(
            contract(cs[g::2], lambda j, h, n: wd_ref[:, at_quarter(q_ref, j, h, n * HALF)], NT), axis=1
        )
        gate, up = gate_ref[rows, :], up_ref[rows, :]
        sig = jax.nn.sigmoid(gate)
        act = gate * sig
        hid_ref[rows, :] = (act * up).astype(BF16)
        gu_ref[rows, :] = (gh * act).astype(BF16)
        gg_ref[rows, :] = (gh * up * sig * (1.0 + gate * (1.0 - sig))).astype(BF16)
    for o_ref, (j, g) in zip(outs, ((2, 0), (2, 1), (1, 1), (3, 0))):
        rows = pl.ds(g * HALF, HALF)
        row_parts(q_ref, gg_ref[rows, :], gu_ref[rows, :], wg_ref, wu_ref, j, o_ref)


def rest_kernel(q_ref, gg_ref, gu_ref, wg_ref, wu_ref, *outs):
    for o_ref, (j, g) in zip(outs, ((1, 0), (3, 1), (0, 0), (0, 1))):
        rows = pl.ds(g * HALF, HALF)
        row_parts(q_ref, gg_ref[rows, :], gu_ref[rows, :], wg_ref, wu_ref, j, o_ref)


def weight_kernel(q_ref, *refs):
    xs, cs, (hid_ref, gu_ref, gg_ref) = refs[:8], refs[8:16], refs[16:19]
    dg_ref, du_ref, dd_ref = refs[19:22]
    moved_ref = refs[22]
    for k, ref in enumerate((hid_ref, gu_ref, gg_ref)):
        moved_ref[k] = moved(ref[:, lanes(1)])

    def last(k, ref, h, rows):
        return ref[rows, lanes(1)] if h == 0 else moved_ref[k, rows, :]

    for j in range(4):
        for h in range(2):
            where = at_quarter(q_ref, j, h)
            dg, du, dd = [], [], []
            for g in range(2):
                rows = pl.ds(g * HALF, HALF)
                x, c = xs[2 * j + g], cs[2 * j + g]
                for part, k in ((lanes(h), 0), (lanes(2), 1)):
                    def of(n, ref):
                        return ref[rows, lanes(0)] if k == 0 else last(n, ref, h, rows)

                    x_t = x[:, part].T
                    dg.append(dot(x_t, of(2, gg_ref)))
                    du.append(dot(x_t, of(1, gu_ref)))
                    dd.append(dot(of(0, hid_ref), c[:, part], TN))
            dg_ref[where, :] = total(dg).astype(BF16)
            du_ref[where, :] = total(du).astype(BF16)
            dd_ref[:, where] = total(dd).astype(BF16)


def local(kernel, q, args, outs, flops, scratch=()):
    return pl.pallas_call(
        kernel,
        in_specs=[pl.BlockSpec(memory_space=pltpu.SMEM)] + whole(len(args)),
        out_specs=whole(len(outs)),
        out_shape=outs,
        scratch_shapes=scratch,
        cost_estimate=pl.CostEstimate(
            flops=flops, transcendentals=0, bytes_accessed=sum(a.size * a.dtype.itemsize for a in args)
        ),
    )(q, *args)


def exchange(buf):
    return lax.all_to_all(buf, "sp", split_axis=0, concat_axis=0, tiled=True)


def gather_quarters(x):
    h0, h1 = jnp.split(x, 2)
    l0, r1 = shift(h0, 1), shift(h1, -1)
    l1, r0 = shift(h1, 1), shift(h0, -1)
    o0, o1 = shift(l0, 1), shift(r1, -1)
    return [h0, h1, r0, r1, o0, o1, l0, l1]


def sum_tp(x):
    a, b, c = shift(x, 1), shift(x, 2), shift(x, -1)
    return (x + a) + (b + c)


def per_device(
    glu_a,
    glu_b,
    saved_conv,
    taps,
    norm_gain_vector,
    out_proj,
    moe_in,
    grad_out,
    expert_ids,
    route_weights,
    w_gate,
    w_up,
    w_down,
):
    n_sp = lax.axis_size("sp")
    tp_pos = lax.axis_index("tp")
    sp_pos = lax.axis_index("sp")
    tok, d_model = grad_out.shape
    quarter = 2 * HALF
    q = tp_pos.reshape(1).astype(jnp.int32)
    wg, wu, wd = w_gate[0], w_up[0], w_down[0]
    rows = n_sp * ROWS
    flop = 2 * rows * HALF * HALF

    in_buf, cot_buf, slots = dispatch(q, expert_ids.T, route_weights.T, moe_in, grad_out, n_sp)
    recv_in = exchange(in_buf.reshape(n_sp, ROWS, WIDE)).reshape(rows, WIDE)
    recv_cot = exchange(cot_buf.reshape(n_sp, ROWS, WIDE)).reshape(rows, WIDE)
    xs = gather_quarters(recv_in)
    cs = gather_quarters(recv_cot)

    f32_rows = jax.ShapeDtypeStruct((rows, 2 * HALF), F32)
    bf_rows = jax.ShapeDtypeStruct((rows, 2 * HALF), BF16)
    bf_part = jax.ShapeDtypeStruct((rows // 2, WIDE), BF16)
    gate, up = local(pre_kernel, q, (*xs, wg, wu), [f32_rows] * 2, 32 * flop)
    hid, gu, gg, p20, p21, p11, p30 = local(
        act_kernel, q, (*cs, wd, wg, wu, gate, up), [bf_rows] * 3 + [bf_part] * 4, 32 * flop
    )
    a0 = shift(p20, 1)
    b1 = shift(p21, -1)
    from_l1 = shift(p11, 1)
    from_r0 = shift(p30, -1)
    p10, p31, p00, p01 = local(rest_kernel, q, (gg, gu, wg, wu), [bf_part] * 4, 16 * flop)
    from_l0 = shift((p10.astype(F32) + a0.astype(F32)).astype(BF16), 1)
    from_r1 = shift((p31.astype(F32) + b1.astype(F32)).astype(BF16), -1)
    own0 = (p00.astype(F32) + from_l0.astype(F32) + from_r0.astype(F32)).astype(BF16)
    own1 = (p01.astype(F32) + from_l1.astype(F32) + from_r1.astype(F32)).astype(BF16)
    own = jnp.concatenate([own0, own1], axis=0)
    returned = exchange(own.reshape(n_sp, ROWS, WIDE)).reshape(rows, WIDE)
    grad_gate, grad_up, grad_down = local(
        weight_kernel,
        q,
        (*xs, *cs, hid, gu, gg),
        [
            jax.ShapeDtypeStruct((d_model, HALF), BF16),
            jax.ShapeDtypeStruct((d_model, HALF), BF16),
            jax.ShapeDtypeStruct((HALF, d_model), BF16),
        ],
        48 * flop,
        [pltpu.VMEM((3, rows, HALF), BF16)],
    )

    conv = saved_conv.astype(F32)
    sums = sum_tp(jnp.stack([jnp.sum(conv, axis=1), jnp.sum(conv * conv, axis=1)]))
    mean = (sums[0] / CONV_CHANNELS)[:, None]
    var = (sums[1] / CONV_CHANNELS)[:, None] - mean * mean
    rstd = lax.rsqrt(var + 1e-05)
    xhat = (conv - mean) * rstd
    normed = xhat * norm_gain_vector[None, :]
    sig = jax.nn.sigmoid(normed)
    heads = (normed * sig).astype(BF16)
    slope = sig * (1.0 + normed * (1.0 - sig)) * norm_gain_vector[None, :]
    heads_all = [heads] + [shift(heads, j) for j in (1, 2, 3)]
    proj = []
    for j in range(4):
        piece = lax.dynamic_slice_in_dim(out_proj, lax.rem(tp_pos + j, 4) * quarter, quarter, 1)
        proj.append(piece if j == 0 else shift(piece, j))
    proj = jnp.concatenate(proj, axis=0)

    slot_a, slot_b, second = slot_ids(jnp.arange(rows, dtype=jnp.int32).astype(F32)[None, :])
    slot0, slot1 = slots[0][:, None], slots[1][:, None]
    pick_a = ((slot0 == slot_a) | (slot1 == slot_a)).astype(BF16)
    hit_b = (slot0 == slot_b) | (slot1 == slot_b)
    pick_b0, pick_b1 = (hit_b & ~second).astype(BF16), (hit_b & second).astype(BF16)
    picked = dot(pick_a, returned[:, : 2 * HALF]) + jnp.concatenate(
        [dot(pick_b0, returned[:, 2 * HALF :]), dot(pick_b1, returned[:, 2 * HALF :])], axis=1
    )
    grad_own = lax.dynamic_slice_in_dim(grad_out, tp_pos * quarter, quarter, 1).astype(F32)
    mix = (grad_own + picked).astype(BF16)

    partial_heads = dot(mix, proj, NT)
    grad_heads = partial_heads[:, :HALF]
    for j in (1, 2, 3):
        grad_heads = grad_heads + shift(partial_heads[:, j * HALF : (j + 1) * HALF].astype(BF16), -j).astype(F32)
    grad_xhat = grad_heads * slope
    sums = sum_tp(jnp.stack([jnp.sum(grad_xhat, axis=1), jnp.sum(grad_xhat * xhat, axis=1)]))
    grad_conv = (
        rstd * (grad_xhat - (sums[0] / CONV_CHANNELS)[:, None] - xhat * (sums[1] / CONV_CHANNELS)[:, None])
    ).astype(BF16)

    reach = (taps.shape[0] - 1) // 2
    pad = reach + 1
    before = lax.ppermute(grad_conv[tok - pad :], "sp", [(i, i + 1) for i in range(n_sp - 1)])
    after = lax.ppermute(grad_conv[:pad], "sp", [(i + 1, i) for i in range(n_sp - 1)])
    padded = jnp.concatenate([before, grad_conv, after], axis=0).astype(F32)
    grad_y = jnp.zeros((tok, HALF), F32)
    for j in range(taps.shape[0]):
        start = pad + reach - j
        grad_y = grad_y + taps[j][None, :] * padded[start : start + tok]
    sig_b = jax.nn.sigmoid(glu_b.astype(F32))
    grad_glu_a = (grad_y * sig_b).astype(BF16)
    grad_glu_b = (grad_y * glu_a.astype(F32) * sig_b * (1.0 - sig_b)).astype(BF16)

    part = jnp.stack([dot(mix, hj, TN).astype(BF16) for hj in heads_all])
    core = lax.rem(sp_pos, 2)
    x_pos = lax.rem(sp_pos // 2, 4)
    n_z = n_sp // 8
    part = part.reshape(4, n_z, 2, 32, HALF)
    keep = lax.dynamic_index_in_dim(part, core, 2, keepdims=False)
    give = lax.dynamic_index_in_dim(part, 1 - core, 2, keepdims=False)
    got = lax.ppermute(give, "sp", [(i, i ^ 1) for i in range(n_sp)])
    part = (keep.astype(F32) + got.astype(F32)).astype(BF16)
    summed = lax.dynamic_index_in_dim(part, x_pos, 0, keepdims=False).astype(F32)
    for d in (1, 2, 3):
        piece = lax.dynamic_index_in_dim(part, lax.rem(x_pos + d, 4), 0, keepdims=False)
        pairs = [(i, (i // 8) * 8 + ((i // 2 + d) % 4) * 2 + i % 2) for i in range(n_sp)]
        summed = summed + lax.ppermute(piece, "sp", pairs).astype(F32)
    blocks = lax.all_to_all(
        summed.astype(BF16),
        "sp",
        split_axis=0,
        concat_axis=0,
        tiled=True,
        axis_index_groups=[[z * 8 + r for z in range(n_z)] for r in range(8)],
    )
    summed = jnp.sum(blocks.astype(F32), axis=0)
    pairs = []
    for s in range(n_sp):
        z, x, c = s // 8, (s // 2) % 4, s % 2
        for t in range(4):
            pairs.append((s * 4 + t, (16 * t + 2 * z + c) * 4 + (t - x) % 4))
    grad_out_proj = lax.ppermute(summed, ("sp", "tp"), pairs)
    return (grad_glu_a, grad_glu_b, grad_out_proj, grad_gate[None], grad_up[None], grad_down[None])


def solution(mesh):
    in_specs = (
        P("sp", "tp"),
        P("sp", "tp"),
        P("sp", "tp"),
        P(None, "tp"),
        P("tp"),
        P("tp", None),
        P("sp", None),
        P("sp", None),
        P("sp", None),
        P("sp", None),
        P("sp", None, "tp"),
        P("sp", None, "tp"),
        P("sp", "tp", None),
    )
    out_specs = (
        P("sp", "tp"),
        P("sp", "tp"),
        P("sp", "tp"),
        P("sp", None, "tp"),
        P("sp", None, "tp"),
        P("sp", "tp", None),
    )

    return jax.shard_map(per_device, mesh=mesh, in_specs=in_specs, out_specs=out_specs, check_vma=False)
```

```python
import jax
import jax.numpy as jnp
from jax import lax
from jax.experimental import pallas as pl
from jax.experimental.pallas import tpu as pltpu
from jax.sharding import PartitionSpec as P


CONV_CHANNELS = 1024
F32 = jnp.float32
BF16 = jnp.bfloat16
CAP = 12
HALF = 256
ROWS = 8
WIDE = 768


NN = (((1,), (0,)), ((), ()))
NT = (((1,), (1,)), ((), ()))
TN = (((0,), (0,)), ((), ()))


def dot(a, b, dims=NN):
    return lax.dot_general(a, b, dims, preferred_element_type=F32)


def swap(x, k):
    return lax.ppermute(x, "tp", [(i, i ^ k) for i in range(4)])


def slot_ids(row):
    e = jnp.floor((row + 0.5) * (1.0 / ROWS))
    r = row - ROWS * e
    second = r >= 4
    return e * CAP + r, e * CAP + 8 + jnp.where(second, r - 4, r), second


def dispatch_kernel(q_ref, ids_ref, w_ref, moe_ref, go_ref, in_ref, cot_ref, slot_ref, own_ref):
    own_ref[...] = go_ref[...]
    n_exp = in_ref.shape[0] // ROWS
    tok = ids_ref.shape[1]
    e_iota = lax.broadcasted_iota(jnp.int32, (n_exp, tok), 0)
    ids0, ids1 = ids_ref[0:1, :], ids_ref[1:2, :]
    oh0 = jnp.where(e_iota == ids0, 1.0, 0.0)
    oh1 = jnp.where(e_iota == ids1, 1.0, 0.0)
    earlier = jnp.where(
        lax.broadcasted_iota(jnp.int32, (tok, tok), 0) < lax.broadcasted_iota(jnp.int32, (tok, tok), 1),
        1.0,
        0.0,
    ).astype(BF16)
    count = dot((oh0 + oh1).astype(BF16), earlier)
    slot0 = ids0.astype(F32) * CAP + jnp.sum(count * oh0, axis=0, keepdims=True)
    slot1 = ids1.astype(F32) * CAP + jnp.sum(count * oh1, axis=0, keepdims=True)
    slot_ref[0:1, :] = slot0
    slot_ref[1:2, :] = slot1
    w0, w1 = w_ref[0:1, :], w_ref[1:2, :]
    step = 256

    @pl.loop(0, in_ref.shape[0] // step)
    def _(i):
        at = pl.multiple_of(i * step, step)
        rows = pl.ds(at, step)
        row = (lax.broadcasted_iota(jnp.int32, (step, tok), 0) + at).astype(F32)
        slot_a, slot_b, second = slot_ids(row)

        def fill(slot, lanes, pick):
            hit0, hit1 = slot == slot0, slot == slot1
            select = jnp.where(hit0 | hit1, 1.0, 0.0).astype(BF16)
            weight = jnp.sum(jnp.where(hit0, w0, 0.0) + jnp.where(hit1, w1, 0.0), axis=1, keepdims=True)
            in_ref[rows, lanes] = pick(dot(select, moe_ref[...])).astype(BF16)
            cot_ref[rows, lanes] = (pick(dot(select, go_ref[...])) * weight).astype(BF16)

        fill(slot_a, pl.ds(0, 2 * HALF), lambda v: v)
        fill(slot_b, pl.ds(2 * HALF, HALF), lambda v: jnp.where(second, v[:, HALF:], v[:, :HALF]))


def dispatch(q, ids_t, w_t, moe_in, grad_out, n_exp):
    tok, _ = moe_in.shape
    rows = n_exp * ROWS
    small = pl.BlockSpec((2, tok), lambda i, q: (0, 0))
    quarter = pl.BlockSpec((tok, 2 * HALF), lambda i, q: (0, q[0]))
    out = pl.BlockSpec((rows, WIDE), lambda i, q: (0, 0))
    return pl.pallas_call(
        dispatch_kernel,
        grid_spec=pltpu.PrefetchScalarGridSpec(
            num_scalar_prefetch=1,
            grid=(1,),
            in_specs=[small, small, quarter, quarter],
            out_specs=[out, out, small, pl.BlockSpec((tok, 2 * HALF), lambda i, q: (0, 0))],
        ),
        out_shape=[
            jax.ShapeDtypeStruct((rows, WIDE), BF16),
            jax.ShapeDtypeStruct((rows, WIDE), BF16),
            jax.ShapeDtypeStruct((2, tok), F32),
            jax.ShapeDtypeStruct((tok, 2 * HALF), BF16),
        ],
        name="dispatch",
    )(q, ids_t, w_t, moe_in, grad_out)


def whole(n):
    return [pl.BlockSpec(memory_space=pltpu.VMEM)] * n


def at_quarter(q_ref, j, h=0, size=HALF):
    return pl.ds(pl.multiple_of(q_ref[j] * (2 * HALF) + h * HALF, HALF), size)


def lanes(k, n=1):
    return pl.ds(k * HALF, n * HALF)


def total(parts):
    out = None
    for p in parts:
        out = p if out is None else out + p
    return out


def roll_rows(x, k):
    return pltpu.roll(x, k % x.shape[0], axis=0)


def lined_up(first, second):
    row = lax.broadcasted_iota(jnp.int32, first.shape, 0)
    return jnp.where((row & 7) < 4, first + roll_rows(second, -4), 0.0)


def contract(xs, w, dims):
    both = total(dot(x[:, lanes(0, 2)], w(j, 0, 2), dims) for j, x in enumerate(xs))
    first = total(dot(x[:, lanes(2)], w(j, 0, 1), dims) for j, x in enumerate(xs))
    second = total(dot(x[:, lanes(2)], w(j, 1, 1), dims) for j, x in enumerate(xs))
    return both, lined_up(first, second)


def pre_kernel(q_ref, *refs):
    xs, (wg_ref, wu_ref, _), (gate_ref, up_ref) = refs[:8], refs[8:11], refs[11:]
    for g in range(2):
        rows = pl.ds(g * HALF, HALF)
        for w_ref, o_ref in ((wg_ref, gate_ref), (wu_ref, up_ref)):
            a, b = contract(xs[g::2], lambda j, h, n: w_ref[at_quarter(q_ref, j, h, n * HALF), :], NN)
            o_ref[rows, lanes(0)] = a
            o_ref[rows, lanes(1)] = b


def row_parts(q_ref, gg, gu, wg_ref, wu_ref, j, o_ref):
    both, h0, h1 = at_quarter(q_ref, j, 0, 2 * HALF), at_quarter(q_ref, j, 0), at_quarter(q_ref, j, 1)
    o_ref[:, lanes(0, 2)] = (
        dot(gg[:, :HALF], wg_ref[both, :], NT) + dot(gu[:, :HALF], wu_ref[both, :], NT)
    ).astype(BF16)
    gg_b, gu_b = gg[:, HALF:], gu[:, HALF:]
    o_ref[:, lanes(2)] = (
        (dot(gg_b, wg_ref[h0, :], NT) + dot(gu_b, wu_ref[h0, :], NT))
        + (dot(moved(gg_b), wg_ref[h1, :], NT) + dot(moved(gu_b), wu_ref[h1, :], NT))
    ).astype(BF16)


def moved(x):
    return roll_rows(x.astype(F32), 4).astype(BF16)


def act_kernel(q_ref, *refs):
    cs, (wd_ref, wg_ref, wu_ref, gate_ref, up_ref) = refs[:8], refs[8:13]
    hid_ref, gu_ref, gg_ref = refs[13:16]
    outs = refs[16:]
    for g in range(2):
        rows = pl.ds(g * HALF, HALF)
        gh = jnp.concatenate(
            contract(cs[g::2], lambda j, h, n: wd_ref[:, at_quarter(q_ref, j, h, n * HALF)], NT), axis=1
        )
        gate, up = gate_ref[rows, :], up_ref[rows, :]
        sig = jax.nn.sigmoid(gate)
        act = gate * sig
        hid_ref[rows, :] = (act * up).astype(BF16)
        gu_ref[rows, :] = (gh * act).astype(BF16)
        gg_ref[rows, :] = (gh * up * sig * (1.0 + gate * (1.0 - sig))).astype(BF16)
    for o_ref, (j, g) in zip(outs, ((2, 0), (2, 1), (1, 0), (3, 1))):
        rows = pl.ds(g * HALF, HALF)
        row_parts(q_ref, gg_ref[rows, :], gu_ref[rows, :], wg_ref, wu_ref, j, o_ref)


def rest_kernel(q_ref, gg_ref, gu_ref, wg_ref, wu_ref, *outs):
    for o_ref, (j, g) in zip(outs, ((3, 0), (1, 1), (0, 0), (0, 1))):
        rows = pl.ds(g * HALF, HALF)
        row_parts(q_ref, gg_ref[rows, :], gu_ref[rows, :], wg_ref, wu_ref, j, o_ref)


def weight_kernel(q_ref, *refs):
    xs, cs, (hid_ref, gu_ref, gg_ref) = refs[:8], refs[8:16], refs[16:19]
    dg_ref, du_ref, dd_ref, last_ref = refs[19:23]
    for k, ref in enumerate((hid_ref, gu_ref, gg_ref)):
        last_ref[0, k] = ref[:, lanes(1)]
        last_ref[1, k] = moved(ref[:, lanes(1)])

    @pl.loop(0, 2)
    def _(h):
        half = pl.ds(pl.multiple_of(h * HALF, HALF), HALF)
        for j in range(4):
            where = pl.ds(pl.multiple_of(q_ref[j] * (2 * HALF) + h * HALF, HALF), HALF)
            dg, du, dd = [], [], []
            for g in range(2):
                rows = pl.ds(g * HALF, HALF)
                x, c = xs[2 * j + g], cs[2 * j + g]
                x_t = x[:, half].T
                dg.append(dot(x_t, gg_ref[rows, lanes(0)]))
                du.append(dot(x_t, gu_ref[rows, lanes(0)]))
                dd.append(dot(hid_ref[rows, lanes(0)], c[:, half], TN))
                x_t = x[:, lanes(2)].T
                dg.append(dot(x_t, last_ref[h, 2, rows, :]))
                du.append(dot(x_t, last_ref[h, 1, rows, :]))
                dd.append(dot(last_ref[h, 0, rows, :], c[:, lanes(2)], TN))
            dg_ref[where, :] = total(dg).astype(BF16)
            du_ref[where, :] = total(du).astype(BF16)
            dd_ref[:, where] = total(dd).astype(BF16)


def row_sums(*arrays):
    rows = [jnp.sum(a.T, axis=0, keepdims=True) for a in arrays]
    return jnp.concatenate(rows + [jnp.zeros((8 - len(rows), rows[0].shape[1]), F32)], axis=0)


def along_lanes(row, n):
    return jnp.broadcast_to(row, (n, row.shape[1])).T


def stats_kernel(q_ref, conv_ref, out_ref):
    conv = conv_ref[...].astype(F32)
    out_ref[...] = row_sums(conv, conv * conv)


def early_kernel(q_ref, *refs):
    conv_ref, gain_ref, slot_ref, proj_ref = refs[:4]
    sums = (refs[4][...] + refs[5][...]) + (refs[6][...] + refs[7][...])
    heads_ref, xhat_ref, slope_ref, rstd_ref, pick_a_ref, pick_b0_ref, pick_b1_ref, own_ref = refs[8:16]
    sends = refs[16:]
    conv = conv_ref[...].astype(F32)
    channels = conv.shape[1]
    mean = sums[0:1, :] / CONV_CHANNELS
    var = sums[1:2, :] / CONV_CHANNELS - mean * mean
    mean = along_lanes(mean, channels)
    rstd = along_lanes(lax.rsqrt(var + 1e-05), channels)
    xhat = (conv - mean) * rstd
    gain = gain_ref[...]
    normed = xhat * gain
    sig = jax.nn.sigmoid(normed)
    heads = (normed * sig).astype(BF16)
    heads_ref[...] = heads
    xhat_ref[...] = xhat
    rstd_ref[...] = rstd
    slope_ref[...] = sig * (1.0 + normed * (1.0 - sig)) * gain
    for j, ref in enumerate((own_ref, *sends)):
        ref[:, lanes(0, 2)] = proj_ref[:, at_quarter(q_ref, j, 0, 2 * HALF)]
        ref[:, lanes(2)] = heads
    rows = pick_a_ref.shape[1]
    slot0, slot1 = along_lanes(slot_ref[0:1, :], rows), along_lanes(slot_ref[1:2, :], rows)
    slot_a, slot_b, second = slot_ids(lax.broadcasted_iota(jnp.int32, slot0.shape, 1).astype(F32))
    hit_b = jnp.where((slot0 == slot_b) | (slot1 == slot_b), 1.0, 0.0)
    pick_a_ref[...] = jnp.where((slot0 == slot_a) | (slot1 == slot_a), 1.0, 0.0).astype(BF16)
    pick_b0_ref[...] = jnp.where(second, 0.0, hit_b).astype(BF16)
    pick_b1_ref[...] = jnp.where(second, hit_b, 0.0).astype(BF16)


def joined_kernel(q_ref, a_ref, b_ref, out_ref):
    out_ref[...] = jnp.zeros(out_ref.shape, F32)


def mix_kernel(q_ref, pick_a_ref, pick_b0_ref, pick_b1_ref, ret_ref, own_ref, *refs):
    msgs, (mix_ref, part_ref) = refs[:4], refs[4:]
    last = ret_ref[:, lanes(2)]
    for h, pick_ref in enumerate((pick_b0_ref, pick_b1_ref)):
        picked = dot(pick_a_ref[...], ret_ref[:, lanes(h)]) + dot(pick_ref[...], last)
        mix_ref[:, lanes(h)] = (own_ref[:, lanes(h)].astype(F32) + picked).astype(BF16)
    for j in range(4):
        part_ref[q_ref[j]] = dot(mix_ref[...], msgs[j][:, lanes(0, 2)], NT).astype(BF16)


def part_kernel(core_ref, mix_ref, *refs):
    msgs, (keep_ref, give_ref, scratch) = refs[:4], refs[4:]
    mix_t = mix_ref[...].T
    core = core_ref[0]
    for j in range(4):
        scratch[...] = dot(mix_t, msgs[j][:, lanes(2)]).astype(BF16)
        for z in range(8):
            keep_ref[4 * z + j] = scratch[pl.ds(pl.multiple_of((2 * z + core) * 32, 32), 32), :]
            give_ref[4 * z + j] = scratch[pl.ds(pl.multiple_of((2 * z + 1 - core) * 32, 32), 32), :]


def xhat_grad_kernel(q_ref, part_ref, slope_ref, xhat_ref, gx_ref, sums_ref):
    grad = total(part_ref[j].astype(F32) for j in range(4)) * slope_ref[...]
    gx_ref[...] = grad
    sums_ref[...] = row_sums(grad, grad * xhat_ref[...])


def conv_grad_kernel(q_ref, gx_ref, xhat_ref, rstd_ref, s0_ref, s1_ref, s2_ref, s3_ref, out_ref, top_ref, low_ref):
    sums = ((s0_ref[...] + s1_ref[...]) + (s2_ref[...] + s3_ref[...])) / CONV_CHANNELS
    channels = gx_ref.shape[1]
    grad_mean = along_lanes(sums[0:1, :], channels)
    product_mean = along_lanes(sums[1:2, :], channels)
    grad = (rstd_ref[...] * (gx_ref[...] - grad_mean - xhat_ref[...] * product_mean)).astype(BF16)
    out_ref[...] = grad
    top_ref[...] = grad[:PAD]
    low_ref[...] = grad[grad.shape[0] - PAD :]


PAD = 16


def glu_kernel(q_ref, before_ref, grad_ref, after_ref, taps_ref, a_ref, b_ref, ga_ref, gb_ref, scratch):
    n = grad_ref.shape[0]
    scratch[0:PAD, :] = before_ref[...].astype(F32)
    scratch[PAD : PAD + n, :] = grad_ref[...].astype(F32)
    scratch[PAD + n :, :] = after_ref[...].astype(F32)
    count = taps_ref.shape[0]
    block = 32
    for at in range(0, n, block):
        rows = pl.ds(at, block)
        grad_y = total(
            taps_ref[j : j + 1, :] * scratch[pl.ds(at + PAD + (count - 1) // 2 - j, block), :] for j in range(count)
        )
        sig = jax.nn.sigmoid(b_ref[rows, :].astype(F32))
        ga_ref[rows, :] = (grad_y * sig).astype(BF16)
        gb_ref[rows, :] = (grad_y * a_ref[rows, :].astype(F32) * sig * (1.0 - sig)).astype(BF16)


def local(kernel, q, args, outs, flops, scratch=(), untouched=False):
    spec = pl.BlockSpec(memory_space=pl.ANY) if untouched else pl.BlockSpec(memory_space=pltpu.VMEM)
    return pl.pallas_call(
        kernel,
        in_specs=[pl.BlockSpec(memory_space=pltpu.SMEM)] + [spec] * len(args),
        out_specs=whole(len(outs)),
        out_shape=[jax.ShapeDtypeStruct(*o) for o in outs],
        scratch_shapes=scratch,
        cost_estimate=pl.CostEstimate(
            flops=flops, transcendentals=0, bytes_accessed=sum(a.size * a.dtype.itemsize for a in args)
        ),
    )(q, *args)


def exchange(buf):
    return lax.all_to_all(buf, "sp", split_axis=0, concat_axis=0, tiled=True)


def gather_quarters(x):
    h0, h1 = jnp.split(x, 2)
    n1_0, n3_1 = swap(h0, 1), swap(h1, 3)
    n1_1, n3_0 = swap(h1, 1), swap(h0, 3)
    o0, o1 = swap(n1_0, 3), swap(n3_1, 1)
    return [h0, h1, n1_0, n1_1, o0, o1, n3_0, n3_1]


def per_device(
    glu_a,
    glu_b,
    saved_conv,
    taps,
    norm_gain_vector,
    out_proj,
    moe_in,
    grad_out,
    expert_ids,
    route_weights,
    w_gate,
    w_up,
    w_down,
):
    n_sp = lax.axis_size("sp")
    tp_pos = lax.axis_index("tp")
    sp_pos = lax.axis_index("sp")
    tok, d_model = grad_out.shape
    q = jnp.stack([tp_pos, tp_pos ^ 1, tp_pos ^ 2, tp_pos ^ 3]).astype(jnp.int32)
    core = lax.rem(sp_pos, 2).reshape(1).astype(jnp.int32)
    wg, wu, wd = w_gate[0], w_up[0], w_down[0]
    rows = n_sp * ROWS
    flop = 2 * rows * HALF * HALF
    square, bf_square = ((tok, HALF), F32), ((tok, HALF), BF16)
    sums8 = ((8, tok), F32)
    small = 1 << 22

    in_buf, cot_buf, slots, grad_own = dispatch(
        q[:1], expert_ids.T, route_weights.T, moe_in, grad_out, n_sp
    )
    recv_in = exchange(in_buf.reshape(n_sp, ROWS, WIDE)).reshape(rows, WIDE)
    recv_cot = exchange(cot_buf.reshape(n_sp, ROWS, WIDE)).reshape(rows, WIDE)

    (sums,) = local(stats_kernel, q, (saved_conv,), [sums8], small)
    all_sums = [sums] + [swap(sums, j) for j in (1, 2, 3)]
    heads, xhat, slope, rstd, pick_a, pick_b0, pick_b1, *msgs = local(
        early_kernel,
        q,
        (saved_conv, norm_gain_vector[None, :], slots, out_proj, *all_sums),
        [bf_square] + [square] * 3 + [((tok, rows), BF16)] * 3 + [((tok, WIDE), BF16)] * 4,
        small,
    )
    msgs = [msgs[0]] + [swap(msgs[j], j) for j in (1, 2, 3)]

    xs = gather_quarters(recv_in)
    (zeros,) = local(joined_kernel, q, (xs[4], xs[5]), [((8, 128), F32)], small, untouched=True)
    cs = gather_quarters(recv_cot)

    f32_rows = ((rows, 2 * HALF), F32)
    bf_rows = ((rows, 2 * HALF), BF16)
    bf_part = ((rows // 2, WIDE), BF16)
    gate, up = local(pre_kernel, q, (*xs, wg, wu, zeros), [f32_rows] * 2, 32 * flop)
    hid, gu, gg, p2_0, p2_1, p1_0, p3_1 = local(
        act_kernel, q, (*cs, wd, wg, wu, gate, up), [bf_rows] * 3 + [bf_part] * 4, 32 * flop
    )
    a0, b1 = swap(p2_0, 1), swap(p2_1, 3)
    direct0, direct1 = swap(p1_0, 1), swap(p3_1, 3)
    p3_0, p1_1, p0_0, p0_1 = local(rest_kernel, q, (gg, gu, wg, wu), [bf_part] * 4, 16 * flop)
    c0 = swap((p3_0.astype(F32) + a0.astype(F32)).astype(BF16), 3)
    c1 = swap((p1_1.astype(F32) + b1.astype(F32)).astype(BF16), 1)
    own0 = (p0_0.astype(F32) + direct0.astype(F32) + c0.astype(F32)).astype(BF16)
    own1 = (p0_1.astype(F32) + direct1.astype(F32) + c1.astype(F32)).astype(BF16)
    own = jnp.concatenate([own0, own1], axis=0)
    returned = exchange(own.reshape(n_sp, ROWS, WIDE)).reshape(rows, WIDE)
    grad_gate, grad_up, grad_down = local(
        weight_kernel,
        q,
        (*xs, *cs, hid, gu, gg),
        [((d_model, HALF), BF16), ((d_model, HALF), BF16), ((HALF, d_model), BF16)],
        48 * flop,
        [pltpu.VMEM((2, 3, rows, HALF), BF16)],
    )

    mix, part = local(
        mix_kernel,
        q,
        (pick_a, pick_b0, pick_b1, returned, grad_own, *msgs),
        [((tok, 2 * HALF), BF16), ((4, tok, HALF), BF16)],
        small,
    )
    part = lax.all_to_all(part, "tp", split_axis=0, concat_axis=0, tiled=True)
    n_z = n_sp // 8
    keep, give = local(
        part_kernel, core, (mix, *msgs), [((4 * n_z, 32, HALF), BF16)] * 2, small, [pltpu.VMEM((2 * HALF, HALF), BF16)]
    )
    got = lax.ppermute(give, "sp", [(i, i ^ 1) for i in range(n_sp)])
    gx, sums = local(xhat_grad_kernel, q, (part, slope, xhat), [square, sums8], small)
    all_sums = [sums] + [swap(sums, j) for j in (1, 2, 3)]
    blocks = lax.all_to_all(
        (keep.astype(F32) + got.astype(F32)).astype(BF16),
        "sp",
        split_axis=0,
        concat_axis=0,
        tiled=True,
        axis_index_groups=[[z * 8 + x * 2 + c for z in range(n_z) for x in range(4)] for c in range(2)],
    )
    grad_conv, top, low = local(
        conv_grad_kernel, q, (gx, xhat, rstd, *all_sums), [bf_square] + [((PAD, HALF), BF16)] * 2, small
    )
    before = lax.ppermute(low, "sp", [(i, i + 1) for i in range(n_sp - 1)])
    after = lax.ppermute(top, "sp", [(i + 1, i) for i in range(n_sp - 1)])
    grad_glu_a, grad_glu_b = local(
        glu_kernel,
        q,
        (before, grad_conv, after, taps, glu_a, glu_b),
        [bf_square] * 2,
        small,
        [pltpu.VMEM((tok + 2 * PAD, HALF), F32)],
    )
    summed = jnp.sum(blocks.astype(F32), axis=0)
    pairs = []
    for s in range(n_sp):
        z, x, c = s // 8, (s // 2) % 4, s % 2
        for t in range(4):
            pairs.append((s * 4 + t, (16 * t + 2 * z + c) * 4 + (t ^ x)))
    grad_out_proj = lax.ppermute(summed, ("sp", "tp"), pairs)
    return (grad_glu_a, grad_glu_b, grad_out_proj, grad_gate[None], grad_up[None], grad_down[None])


def solution(mesh):
    in_specs = (
        P("sp", "tp"),
        P("sp", "tp"),
        P("sp", "tp"),
        P(None, "tp"),
        P("tp"),
        P("tp", None),
        P("sp", None),
        P("sp", None),
        P("sp", None),
        P("sp", None),
        P("sp", None, "tp"),
        P("sp", None, "tp"),
        P("sp", "tp", None),
    )
    out_specs = (
        P("sp", "tp"),
        P("sp", "tp"),
        P("sp", "tp"),
        P("sp", None, "tp"),
        P("sp", None, "tp"),
        P("sp", "tp", None),
    )

    return jax.shard_map(per_device, mesh=mesh, in_specs=in_specs, out_specs=out_specs, check_vma=False)
```
